1024 devices in a mesh: ra: 128 (over z, y), cb: 8 (over x, core).
Axes of the slice: x: 4, y: 8, z: 16, core: 2. Of those that a mesh axis runs over, the one named last changes fastest.
Arguments:
- tokens: bfloat16 [512, 4096], P(None, 'cb'), may hold values from -82 to 82
- gate_weight: float32 [2, 4096, 11264], P(None, 'cb', 'ra'), may hold values from -0.09375 to 0.09375
- up_weight: float32 [2, 4096, 11264], P(None, 'cb', 'ra'), may hold values from -0.09375 to 0.09375
- down_weight: float32 [2, 11264, 4096], P(None, 'ra', 'cb'), may hold values from -0.0546875 to 0.0546875
- gate_scale: float32 [2, 11264], P(None, 'ra'), may hold values from 0.5 to 2
- up_scale: float32 [2, 11264], P(None, 'ra'), may hold values from 0.5 to 2
- down_scale: float32 [2, 4096], P(None, 'cb'), may hold values from 0.5 to 2
- norm_gain: float32 [2, 4096], P(None, 'cb'), may hold values from 0.1 to 1.9
- conv_taps: float32 [2, 3, 11264], P(None, None, 'ra'), may hold values from -3 to 3
- conv_bias: float32 [2, 11264], P(None, 'ra'), may hold values from -3 to 3
Outputs:
- layer_out: bfloat16 [512, 4096], P(None, 'cb')
The draws below stay inside these ranges and needn't reach their ends.
All inputs are finite; a program needn't handle non-finite values.
Results may differ from the reference program's by a relative error of at most 0.012.
Values may be sent and summed in bfloat16 or wider, within the bound.
No kernel may reach another device: no remote copies, remote signals or barrier semaphores. Data moves between devices by JAX's collectives and lax.ppermute only.
A program may use at most 32 MiB of HBM per device.

```python
import math
import jax
import jax.numpy as jnp
from jax import lax

D = 4096
FF = 11264
TOKENS = 512
LAYERS = 2
KERNEL = 3


def draw_tokens(key, part):
    k_base, k_row, k_col = jax.random.split(key, 3)
    trend = jnp.linspace(0.0, math.log(10.0), D)
    jitter = jax.random.uniform(k_col, (D,), jnp.float32, -0.3, 0.3)
    column = jnp.exp(trend + jitter)
    row_scale = jnp.exp(jax.random.uniform(k_row, (TOKENS, 1), jnp.float32, 0.0, math.log(10.0)))
    base = jnp.clip(jax.random.normal(k_base, (TOKENS, D), jnp.float32), -6.0, 6.0)
    values = base * row_scale * column * 0.1
    return values.astype(jnp.bfloat16)


def level_of(own_key, shape, cuts, least, high):
    level, own = 1.0, jax.random.fold_in(own_key, 6)
    for axis_at, parts in cuts:
        steps = jnp.exp(jax.random.uniform(jax.random.fold_in(own, axis_at), (parts,), jnp.float32, least / len(cuts), high / len(cuts)))
        level = level * jnp.repeat(steps, shape[axis_at] // parts).reshape([-1 if axis == axis_at else 1 for axis in range(len(shape))])
    return level


def normal_values(stream_key, shape, width, bound, cuts=(), dtype=jnp.bfloat16):
    array = jax.random.normal(stream_key, shape, jnp.float32) * width
    if len(cuts) > 0:
        array = level_of(stream_key, shape, cuts, -0.22, 0.18) * array
    return jnp.clip(array, min=-bound, max=bound).astype(dtype)


def setup_inputs(seed: int = 0) -> dict:
    streams_of = jax.random.split(jax.random.key(seed), 11)
    return {
        "tokens": draw_tokens(jax.random.fold_in(streams_of[10], 71), 0),
        "gate_weight": normal_values(streams_of[1], (LAYERS, D, FF), D ** -0.5, 0.09375, ((1, 8), (2, 128)), jnp.float32),
        "up_weight": normal_values(streams_of[2], (LAYERS, D, FF), D ** -0.5, 0.09375, ((1, 8), (2, 128)), jnp.float32),
        "down_weight": normal_values(streams_of[3], (LAYERS, FF, D), FF ** -0.5, 0.0546875, ((1, 128), (2, 8)), jnp.float32),
        "gate_scale": jnp.clip(jnp.exp(math.log(2.0) - 1.3862944 * jax.random.uniform(streams_of[4], (LAYERS, FF), jnp.float32) ** level_of(streams_of[4], (LAYERS, FF), ((1, 128),), -0.2, 0.2)), 0.5, 2.0),
        "up_scale": jnp.clip(jnp.exp(math.log(2.0) - 1.3862944 * jax.random.uniform(streams_of[5], (LAYERS, FF), jnp.float32) ** level_of(streams_of[5], (LAYERS, FF), ((1, 128),), -0.2, 0.2)), 0.5, 2.0),
        "down_scale": jnp.clip(jnp.exp(math.log(2.0) - 1.3862944 * jax.random.uniform(streams_of[6], (LAYERS, D), jnp.float32) ** level_of(streams_of[6], (LAYERS, D), ((1, 8),), -0.2, 0.2)), 0.5, 2.0),
        "norm_gain": jnp.clip(1.0 + 0.18 * jax.random.normal(streams_of[7], (LAYERS, D), jnp.float32), 0.1, 1.9),
        "conv_taps": normal_values(streams_of[8], (LAYERS, KERNEL, FF), 0.6, 3.0, ((2, 128),), jnp.float32),
        "conv_bias": normal_values(streams_of[9], (LAYERS, FF), 0.5, 3.0, ((1, 128),), jnp.float32),
    }


norm_eps = 1e-06
residual_scale = 0.25

def reference(tokens, gate_weight, up_weight, down_weight, gate_scale, up_scale, down_scale, norm_gain, conv_taps, conv_bias):
    hstate = tokens
    for layer in range(LAYERS):
        wide = hstate.astype(jnp.float32)
        stat = lax.optimization_barrier(jnp.mean(wide * wide, axis=1, keepdims=True))
        rscale = lax.rsqrt(stat + norm_eps)
        operand = (wide * norm_gain[layer]).astype(jnp.bfloat16)
        gate = jnp.dot(operand, gate_weight[layer].astype(jnp.bfloat16), preferred_element_type=jnp.float32) * rscale * gate_scale[layer]
        upward = jnp.dot(operand, up_weight[layer].astype(jnp.bfloat16), preferred_element_type=jnp.float32) * rscale * up_scale[layer]
        taps = conv_taps[layer]
        padded = jnp.pad(gate, ((1, 1), (0, 0)))
        mixed = taps[0] * padded[:-2] + taps[1] * padded[1:-1] + taps[2] * padded[2:] + conv_bias[layer]
        hidden = (jax.nn.silu(mixed) * upward).astype(jnp.bfloat16)
        branch = jnp.dot(hidden, down_weight[layer].astype(jnp.bfloat16), preferred_element_type=jnp.float32) * down_scale[layer]
        hstate = (residual_scale * wide + branch).astype(jnp.bfloat16)
    return hstate
```

```python
import jax
import jax.numpy as jnp
from jax import lax
from jax.sharding import Mesh
from jax.sharding import PartitionSpec as P

RA = ("ra_0", "ra_1")
LANES = 128
TILE = 8

norm_eps = 1e-06
residual_scale = 0.25


def swapped(pieces, axes):
    return lax.all_to_all(pieces, axes, 0, 0, tiled=True)


def sent_to_all(value, axes):
    return swapped(jnp.broadcast_to(value[None], (lax.axis_size(axes), *value.shape)), axes)


def padded_to(value, size, axis):
    widths = [(0, 0)] * value.ndim
    widths[axis] = (0, size - value.shape[axis])
    return jnp.pad(value, widths)


def with_neighbours(rows, blocks):
    width = rows.shape[1]
    main = rows.reshape(blocks, -1, width)
    nothing = jnp.zeros((1, width), rows.dtype)
    before = jnp.concatenate([nothing, main[:-1, -1]], axis=0)[:, None]
    after = jnp.concatenate([main[1:, 0], nothing], axis=0)[:, None]
    rest = jnp.zeros((blocks, TILE - 2, width), rows.dtype)
    return jnp.concatenate([main, before, after, rest], axis=1)


def split_in_two(value):
    high = lax.reduce_precision(value, 8, 7)
    return high, value - high


def split_in_three(value):
    first, rest = split_in_two(value)
    second, third = split_in_two(rest)
    return jnp.concatenate([first, second, third], axis=0).astype(jnp.bfloat16)


def side_by_side(gate_weight, up_weight):
    return jnp.concatenate(
        [padded_to(gate_weight, LANES, 1), padded_to(up_weight, LANES, 1)], axis=1
    ).astype(jnp.bfloat16)


def with_squares(product, squares, hidden):
    high, low = split_in_two(squares)
    column = lax.broadcasted_iota(jnp.int32, product.shape, product.ndim - 1)
    product = jnp.where(column == hidden, high, product)
    return jnp.where(column == hidden + 1, low, product)


def activated(total, features, hidden, params):
    rows = total.shape[0] - TILE
    square_sum = total[:, hidden : hidden + 1] + total[:, hidden + 1 : hidden + 2]
    rscale = lax.rsqrt(square_sum / features + norm_eps)
    gate = total[:, :LANES] * rscale * params[4]
    upward = total[:rows, LANES:] * rscale[:rows] * params[5]
    main = gate[:rows]
    before = jnp.concatenate([gate[rows : rows + 1], main[:-1]], axis=0)
    after = jnp.concatenate([main[1:], gate[rows + 1 : rows + 2]], axis=0)
    mixed = params[0] * before + params[1] * main + params[2] * after + params[3]
    return (jax.nn.silu(mixed) * upward).astype(jnp.bfloat16)


def own_params(conv_taps, conv_bias, gate_scale, up_scale):
    stacked = jnp.concatenate([conv_taps, conv_bias[None], gate_scale[None], up_scale[None]], axis=0)
    return padded_to(stacked, LANES, 1)


def per_device(
    tokens,
    gate_weight,
    up_weight,
    down_weight,
    gate_scale,
    up_scale,
    down_scale,
    norm_gain,
    conv_taps,
    conv_bias,
):
    blocks_c, blocks_y, blocks_z = (lax.axis_size(a) for a in ("cb", "ra_1", "ra_0"))
    at_y, at_z = lax.axis_index("ra_1"), lax.axis_index("ra_0")
    length, width = tokens.shape
    hidden = gate_weight.shape[2]
    features = width * blocks_c
    block = length // blocks_y
    f32, bf16 = jnp.float32, jnp.bfloat16

    params_1 = own_params(conv_taps[1], conv_bias[1], gate_scale[1], up_scale[1])
    carried = split_in_three(padded_to(params_1, TILE, 0))
    carried = padded_to(carried, 2 * LANES, 1)
    packed = jnp.concatenate([side_by_side(gate_weight[1], up_weight[1]), carried], axis=0)
    packed = lax.all_gather(packed, "ra_1", axis=0)
    down_1 = lax.all_gather(padded_to(down_weight[1], LANES, 0).astype(bf16), "ra_1", axis=0)

    params_0 = own_params(conv_taps[0], conv_bias[0], gate_scale[0], up_scale[0])
    wide = tokens.astype(f32)
    squares = jnp.sum(wide * wide, axis=1, keepdims=True)
    operand = (wide * norm_gain[0]).astype(bf16)
    product = jnp.dot(
        operand, side_by_side(gate_weight[0], up_weight[0]), preferred_element_type=f32
    )
    product = with_squares(product, squares, hidden).astype(bf16)
    total = swapped(with_neighbours(product, blocks_c), "cb").astype(f32).sum(axis=0)
    inner = activated(total, features, hidden, params_0)
    inner = sent_to_all(inner, "cb").reshape(length, LANES)
    down_0 = padded_to(down_weight[0], LANES, 0).astype(bf16)
    term = jnp.dot(inner, down_0, preferred_element_type=f32).astype(bf16)
    part = swapped(with_neighbours(term, blocks_y), "ra_1").astype(f32).sum(axis=0)
    share_rows = TILE
    part = padded_to(part.astype(bf16), share_rows * blocks_z, 0)
    part = swapped(part.reshape(blocks_z, share_rows, width), "ra_0").astype(f32).sum(axis=0)

    start = block * at_y
    mains = block // share_rows
    own = lax.dynamic_slice_in_dim(tokens, start + share_rows * jnp.minimum(at_z, mains - 1), share_rows, 0)
    before = lax.dynamic_slice_in_dim(tokens, jnp.maximum(start - 1, 0), 1, 0)
    after = lax.dynamic_slice_in_dim(tokens, jnp.minimum(start + block, length - 1), 1, 0)
    row = lax.broadcasted_iota(jnp.int32, (share_rows, 1), 0)
    edge = jnp.where((row == 0) & (at_y > 0), before, jnp.zeros_like(before))
    edge = jnp.where((row == 1) & (at_y < blocks_y - 1), after, edge)
    own = jnp.where(at_z < mains, own, jnp.where(at_z == mains, edge, jnp.zeros_like(edge)))
    fresh = (residual_scale * own.astype(f32) + part * down_scale[0]).astype(bf16)
    hstate = sent_to_all(fresh, "ra_0").reshape(blocks_z * share_rows, width)[: block + TILE]

    wide = hstate.astype(f32)
    squares = jnp.sum(wide * wide, axis=1, keepdims=True)
    operand = (wide * norm_gain[1]).astype(bf16)
    product = jnp.einsum("td,ydk->ytk", operand, packed[:, :width], preferred_element_type=f32)
    product = with_squares(product, squares[None], hidden).astype(bf16)
    total = swapped(product, "cb").astype(f32).sum(axis=0)
    theirs = lax.dynamic_index_in_dim(packed, lax.axis_index("cb"), 0, keepdims=False)
    theirs = theirs[width:, :LANES].astype(f32).reshape(3, TILE, LANES)
    theirs = theirs[0] + theirs[1] + theirs[2]
    inner = activated(total, features, hidden, theirs)
    inner = sent_to_all(inner, "cb")
    term = jnp.einsum("ytk,ykf->tf", inner, down_1, preferred_element_type=f32).astype(bf16)
    share_rows = block // blocks_z
    part = swapped(term.reshape(blocks_z, share_rows, width), "ra_0").astype(f32).sum(axis=0)
    own = lax.dynamic_slice_in_dim(hstate, share_rows * at_z, share_rows, 0).astype(f32)
    fresh = (residual_scale * own + part * down_scale[1]).astype(bf16)
    fresh = sent_to_all(fresh, "ra_0").reshape(block, width)
    return sent_to_all(fresh, "ra_1").reshape(length, width)


def solution(mesh):
    split = Mesh(mesh.devices.reshape(16, 8, mesh.shape["cb"]), ("ra_0", "ra_1", "cb"))
    return jax.shard_map(
        per_device,
        mesh=split,
        in_specs=(
            P(None, "cb"),
            P(None, "cb", RA),
            P(None, "cb", RA),
            P(None, RA, "cb"),
            P(None, RA),
            P(None, RA),
            P(None, "cb"),
            P(None, "cb"),
            P(None, None, RA),
            P(None, RA),
        ),
        out_specs=P(None, "cb"),
        check_vma=False,
    )
```

```python
import jax
import jax.numpy as jnp
from jax import lax
from jax.sharding import Mesh
from jax.sharding import PartitionSpec as P

RA = ("ra_0", "ra_1")
LANES = 128
TILE = 8

norm_eps = 1e-06
residual_scale = 0.25


def swapped(pieces, axes):
    return lax.all_to_all(pieces, axes, 0, 0, tiled=True)


def sent_to_all(value, axes):
    return swapped(jnp.broadcast_to(value[None], (lax.axis_size(axes), *value.shape)), axes)


def padded_to(value, size, axis):
    widths = [(0, 0)] * value.ndim
    widths[axis] = (0, size - value.shape[axis])
    return jnp.pad(value, widths)


def with_neighbours(rows, blocks):
    width = rows.shape[1]
    main = rows.reshape(blocks, -1, width)
    nothing = jnp.zeros((1, width), rows.dtype)
    before = jnp.concatenate([nothing, main[:-1, -1]], axis=0)[:, None]
    after = jnp.concatenate([main[1:, 0], nothing], axis=0)[:, None]
    rest = jnp.zeros((blocks, TILE - 2, width), rows.dtype)
    return jnp.concatenate([main, before, after, rest], axis=1)


def split_in_two(value):
    high = lax.reduce_precision(value, 8, 7)
    return high, value - high


def split_in_three(value):
    first, rest = split_in_two(value)
    second, third = split_in_two(rest)
    return jnp.concatenate([first, second, third], axis=0).astype(jnp.bfloat16)


def side_by_side(gate_weight, up_weight):
    return jnp.concatenate(
        [padded_to(gate_weight, LANES, 1), padded_to(up_weight, LANES, 1)], axis=1
    ).astype(jnp.bfloat16)


def with_squares(product, squares, hidden):
    high, low = split_in_two(squares)
    column = lax.broadcasted_iota(jnp.int32, product.shape, product.ndim - 1)
    product = jnp.where(column == hidden, high, product)
    return jnp.where(column == hidden + 1, low, product)


def activated(total, features, hidden, params):
    rows = total.shape[0] - TILE
    square_sum = total[:, hidden : hidden + 1] + total[:, hidden + 1 : hidden + 2]
    rscale = lax.rsqrt(square_sum / features + norm_eps)
    gate = total[:, :LANES] * rscale * params[4]
    upward = total[:rows, LANES:] * rscale[:rows] * params[5]
    main = gate[:rows]
    before = jnp.concatenate([gate[rows : rows + 1], main[:-1]], axis=0)
    after = jnp.concatenate([main[1:], gate[rows + 1 : rows + 2]], axis=0)
    mixed = params[0] * before + params[1] * main + params[2] * after + params[3]
    return (jax.nn.silu(mixed) * upward).astype(jnp.bfloat16)


def own_params(conv_taps, conv_bias, gate_scale, up_scale):
    stacked = jnp.concatenate([conv_taps, conv_bias[None], gate_scale[None], up_scale[None]], axis=0)
    return padded_to(stacked, LANES, 1)


def per_device(
    tokens,
    gate_weight,
    up_weight,
    down_weight,
    gate_scale,
    up_scale,
    down_scale,
    norm_gain,
    conv_taps,
    conv_bias,
):
    blocks_c, blocks_y, blocks_z = (lax.axis_size(a) for a in ("cb", "ra_1", "ra_0"))
    at_y, at_z = lax.axis_index("ra_1"), lax.axis_index("ra_0")
    length, width = tokens.shape
    hidden = gate_weight.shape[2]
    features = width * blocks_c
    block = length // blocks_y
    f32, bf16 = jnp.float32, jnp.bfloat16

    params_1 = own_params(conv_taps[1], conv_bias[1], gate_scale[1], up_scale[1])
    carried = padded_to(split_in_three(padded_to(params_1, TILE, 0)), width, 1)
    packed = jnp.concatenate(
        [
            gate_weight[1].T.astype(bf16),
            up_weight[1].T.astype(bf16),
            down_weight[1].astype(bf16),
            carried,
        ],
        axis=0,
    )
    packed = lax.all_gather(packed, "ra_1", axis=0)

    params_0 = own_params(conv_taps[0], conv_bias[0], gate_scale[0], up_scale[0])
    wide = tokens.astype(f32)
    squares = jnp.sum(wide * wide, axis=1, keepdims=True)
    operand = (wide * norm_gain[0]).astype(bf16)
    product = jnp.dot(
        operand, side_by_side(gate_weight[0], up_weight[0]), preferred_element_type=f32
    )
    product = with_squares(product, squares, hidden).astype(bf16)
    total = swapped(with_neighbours(product, blocks_c), "cb").astype(f32).sum(axis=0)
    inner = activated(total, features, hidden, params_0)
    inner = sent_to_all(inner, "cb").reshape(length, LANES)
    down_0 = padded_to(down_weight[0], LANES, 0).astype(bf16)
    term = jnp.dot(inner, down_0, preferred_element_type=f32).astype(bf16)
    part = swapped(with_neighbours(term, blocks_y), "ra_1").astype(f32).sum(axis=0)
    share_rows = TILE
    part = padded_to(part.astype(bf16), share_rows * blocks_z, 0)
    part = swapped(part.reshape(blocks_z, share_rows, width), "ra_0").astype(f32).sum(axis=0)

    start = block * at_y
    mains = block // share_rows
    own = lax.dynamic_slice_in_dim(tokens, start + share_rows * jnp.minimum(at_z, mains - 1), share_rows, 0)
    before = lax.dynamic_slice_in_dim(tokens, jnp.maximum(start - 1, 0), 1, 0)
    after = lax.dynamic_slice_in_dim(tokens, jnp.minimum(start + block, length - 1), 1, 0)
    row = lax.broadcasted_iota(jnp.int32, (share_rows, 1), 0)
    edge = jnp.where((row == 0) & (at_y > 0), before, jnp.zeros_like(before))
    edge = jnp.where((row == 1) & (at_y < blocks_y - 1), after, edge)
    own = jnp.where(at_z < mains, own, jnp.where(at_z == mains, edge, jnp.zeros_like(edge)))
    fresh = (residual_scale * own.astype(f32) + part * down_scale[0]).astype(bf16)
    hstate = sent_to_all(fresh, "ra_0").reshape(blocks_z * share_rows, width)[: block + TILE]

    wide = hstate.astype(f32)
    squares = jnp.sum(wide * wide, axis=1, keepdims=True)
    operand = (wide * norm_gain[1]).astype(bf16)
    product = jnp.concatenate(
        [
            padded_to(
                jnp.einsum("td,ykd->ytk", operand, weight, preferred_element_type=f32), LANES, 2
            )
            for weight in (packed[:, :hidden], packed[:, hidden : 2 * hidden])
        ],
        axis=2,
    )
    product = with_squares(product, squares[None], hidden).astype(bf16)
    total = swapped(product, "cb").astype(f32).sum(axis=0)
    theirs = lax.dynamic_index_in_dim(packed, lax.axis_index("cb"), 0, keepdims=False)
    theirs = theirs[3 * hidden :, :LANES].astype(f32).reshape(3, TILE, LANES)
    theirs = theirs[0] + theirs[1] + theirs[2]
    inner = activated(total, features, hidden, theirs)
    inner = sent_to_all(inner, "cb")
    down_1 = packed[:, 2 * hidden : 3 * hidden]
    term = jnp.einsum("ytk,ykf->tf", inner[:, :, :hidden], down_1, preferred_element_type=f32)
    term = term.astype(bf16)
    share_rows = block // blocks_z
    part = swapped(term.reshape(blocks_z, share_rows, width), "ra_0").astype(f32).sum(axis=0)
    own = lax.dynamic_slice_in_dim(hstate, share_rows * at_z, share_rows, 0).astype(f32)
    fresh = (residual_scale * own + part * down_scale[1]).astype(bf16)
    fresh = sent_to_all(fresh, "ra_0").reshape(block, width)
    return sent_to_all(fresh, "ra_1").reshape(length, width)


def solution(mesh):
    split = Mesh(mesh.devices.reshape(16, 8, mesh.shape["cb"]), ("ra_0", "ra_1", "cb"))
    return jax.shard_map(
        per_device,
        mesh=split,
        in_specs=(
            P(None, "cb"),
            P(None, "cb", RA),
            P(None, "cb", RA),
            P(None, RA, "cb"),
            P(None, RA),
            P(None, RA),
            P(None, "cb"),
            P(None, "cb"),
            P(None, None, RA),
            P(None, RA),
        ),
        out_specs=P(None, "cb"),
        check_vma=False,
    )
```

```python
import jax
import jax.numpy as jnp
from jax import lax
from jax.sharding import Mesh
from jax.sharding import PartitionSpec as P


RA = ("ra_0", "ra_1")
LANES = 128
TILE = 8

norm_eps = 1e-06
residual_scale = 0.25


def swapped(pieces, axes):
    return lax.all_to_all(pieces, axes, 0, 0, tiled=True)


def sent_to_all(value, axes):
    return swapped(jnp.broadcast_to(value[None], (lax.axis_size(axes), *value.shape)), axes)


def padded_to(value, size, axis):
    widths = [(0, 0)] * value.ndim
    widths[axis] = (0, size - value.shape[axis])
    return jnp.pad(value, widths)


def with_neighbours(rows, blocks):
    width = rows.shape[1]
    main = rows.reshape(blocks, -1, width)
    nothing = jnp.zeros((1, width), rows.dtype)
    before = jnp.concatenate([nothing, main[:-1, -1]], axis=0)[:, None]
    after = jnp.concatenate([main[1:, 0], nothing], axis=0)[:, None]
    rest = jnp.zeros((blocks, TILE - 2, width), rows.dtype)
    return jnp.concatenate([main, before, after, rest], axis=1)


def split_in_two(value):
    high = lax.reduce_precision(value, 8, 7)
    return high, value - high


def split_in_three(value):
    first, rest = split_in_two(value)
    second, third = split_in_two(rest)
    return jnp.concatenate([first, second, third], axis=0).astype(jnp.bfloat16)


def side_by_side(gate_weight, up_weight):
    return jnp.concatenate(
        [padded_to(gate_weight, LANES, 1), padded_to(up_weight, LANES, 1)], axis=1
    ).astype(jnp.bfloat16)


def with_squares(product, squares, hidden):
    high, low = split_in_two(squares)
    column = lax.broadcasted_iota(jnp.int32, product.shape, product.ndim - 1)
    product = jnp.where(column == hidden, high, product)
    return jnp.where(column == hidden + 1, low, product)


def activated(total, features, hidden, params):
    rows = total.shape[0] - TILE
    square_sum = total[:, hidden : hidden + 1] + total[:, hidden + 1 : hidden + 2]
    rscale = lax.rsqrt(square_sum / features + norm_eps)
    gate = total[:, :LANES] * rscale * params[4]
    upward = total[:rows, LANES:] * rscale[:rows] * params[5]
    main = gate[:rows]
    before = jnp.concatenate([gate[rows : rows + 1], main[:-1]], axis=0)
    after = jnp.concatenate([main[1:], gate[rows + 1 : rows + 2]], axis=0)
    mixed = params[0] * before + params[1] * main + params[2] * after + params[3]
    return (jax.nn.silu(mixed) * upward).astype(jnp.bfloat16)


def own_params(conv_taps, conv_bias, gate_scale, up_scale):
    stacked = jnp.concatenate([conv_taps, conv_bias[None], gate_scale[None], up_scale[None]], axis=0)
    return padded_to(stacked, LANES, 1)


def per_device(
    tokens,
    gate_weight,
    up_weight,
    down_weight,
    gate_scale,
    up_scale,
    down_scale,
    norm_gain,
    conv_taps,
    conv_bias,
):
    blocks_c, blocks_y, blocks_z = (lax.axis_size(a) for a in ("cb", "ra_1", "ra_0"))
    at_y, at_z = lax.axis_index("ra_1"), lax.axis_index("ra_0")
    length, width = tokens.shape
    hidden = gate_weight.shape[2]
    features = width * blocks_c
    block = length // blocks_y
    f32, bf16 = jnp.float32, jnp.bfloat16

    params_1 = own_params(conv_taps[1], conv_bias[1], gate_scale[1], up_scale[1])
    carried = padded_to(split_in_three(padded_to(params_1, TILE, 0)), width, 1)
    packed = jnp.concatenate(
        [
            gate_weight[1].T.astype(bf16),
            up_weight[1].T.astype(bf16),
            down_weight[1].astype(bf16),
            carried,
        ],
        axis=0,
    )
    packed = lax.all_gather(packed, "ra_1", axis=0)

    params_0 = own_params(conv_taps[0], conv_bias[0], gate_scale[0], up_scale[0])
    wide = tokens.astype(f32)
    squares = jnp.sum(wide * wide, axis=1, keepdims=True)
    operand = (wide * norm_gain[0]).astype(bf16)
    product = jnp.dot(
        operand, side_by_side(gate_weight[0], up_weight[0]), preferred_element_type=f32
    )
    product = with_squares(product, squares, hidden).astype(bf16)
    total = swapped(with_neighbours(product, blocks_c), "cb").astype(f32).sum(axis=0)
    inner = activated(total, features, hidden, params_0)
    inner = sent_to_all(inner, "cb").reshape(length, LANES)
    down_0 = padded_to(down_weight[0], LANES, 0).astype(bf16)
    term = jnp.dot(inner, down_0, preferred_element_type=f32).astype(bf16)

    halves = 2
    groups = blocks_z // halves
    share_rows, half = block // groups, width // halves
    term = term.reshape(blocks_y, groups, share_rows, halves, half).transpose(1, 3, 0, 2, 4)
    part = swapped(term.reshape(blocks_z, blocks_y * share_rows, half), "ra_0")
    part = part.astype(f32).sum(axis=0).astype(bf16)
    part = swapped(with_neighbours(part, blocks_y), "ra_1").astype(f32).sum(axis=0)
    group, column = at_z // halves, (at_z % halves) * half

    def residual_rows(block_at, row, count):
        start = jnp.clip(block_at, 0, blocks_y - 1) * block + group * share_rows + row
        rows = lax.dynamic_slice(tokens, (start, column), (count, half))
        inside = (block_at >= 0) & (block_at < blocks_y)
        return jnp.where(inside, rows, jnp.zeros_like(rows))

    own = jnp.concatenate(
        [
            residual_rows(at_y, 0, share_rows),
            residual_rows(at_y - 1, share_rows - 1, 1),
            residual_rows(at_y + 1, 0, 1),
            jnp.zeros((TILE - 2, half), bf16),
        ],
        axis=0,
    )
    scale = lax.dynamic_slice_in_dim(down_scale[0], column, half, 0)
    fresh = (residual_scale * own.astype(f32) + part * scale).astype(bf16)
    fresh = sent_to_all(fresh, "ra_0").reshape(groups, halves, share_rows + TILE, half)
    rows = fresh[:, :, :share_rows].transpose(0, 2, 1, 3).reshape(block, width)
    before = fresh[groups - 1, :, share_rows].reshape(1, width)
    after = fresh[0, :, share_rows + 1].reshape(1, width)
    hstate = jnp.concatenate([rows, before, after, jnp.zeros((TILE - 2, width), bf16)], axis=0)

    wide = hstate.astype(f32)
    squares = jnp.sum(wide * wide, axis=1, keepdims=True)
    operand = (wide * norm_gain[1]).astype(bf16)
    product = jnp.concatenate(
        [
            padded_to(
                jnp.einsum("td,ykd->ytk", operand, weight, preferred_element_type=f32), LANES, 2
            )
            for weight in (packed[:, :hidden], packed[:, hidden : 2 * hidden])
        ],
        axis=2,
    )
    product = with_squares(product, squares[None], hidden).astype(bf16)
    total = swapped(product, "cb").astype(f32).sum(axis=0)
    theirs = lax.dynamic_index_in_dim(packed, lax.axis_index("cb"), 0, keepdims=False)
    theirs = theirs[3 * hidden :, :LANES].astype(f32).reshape(3, TILE, LANES)
    theirs = theirs[0] + theirs[1] + theirs[2]
    inner = activated(total, features, hidden, theirs)
    inner = sent_to_all(inner, "cb")
    down_1 = packed[:, 2 * hidden : 3 * hidden]
    term = jnp.einsum("ytk,ykf->tf", inner[:, :, :hidden], down_1, preferred_element_type=f32)
    term = term.astype(bf16)
    share_rows = block // blocks_z
    part = swapped(term.reshape(blocks_z, share_rows, width), "ra_0").astype(f32).sum(axis=0)
    own = lax.dynamic_slice_in_dim(hstate, share_rows * at_z, share_rows, 0).astype(f32)
    fresh = (residual_scale * own + part * down_scale[1]).astype(bf16)
    fresh = sent_to_all(fresh, "ra_0").reshape(block, width)
    return sent_to_all(fresh, "ra_1").reshape(length, width)


def solution(mesh):
    split = Mesh(mesh.devices.reshape(16, 8, mesh.shape["cb"]), ("ra_0", "ra_1", "cb"))
    return jax.shard_map(
        per_device,
        mesh=split,
        in_specs=(
            P(None, "cb"),
            P(None, "cb", RA),
            P(None, "cb", RA),
            P(None, RA, "cb"),
            P(None, RA),
            P(None, RA),
            P(None, "cb"),
            P(None, "cb"),
            P(None, None, RA),
            P(None, RA),
        ),
        out_specs=P(None, "cb"),
        check_vma=False,
    )
```

```python
import jax
import jax.numpy as jnp
from jax import lax
from jax.sharding import Mesh
from jax.sharding import PartitionSpec as P


RA = ("ra_0", "ra_1")
LANES = 128
TILE = 8

norm_eps = 1e-06
residual_scale = 0.25


def swapped(pieces, axes):
    return lax.all_to_all(pieces, axes, 0, 0, tiled=True)


def sent_to_all(value, axes):
    copies = jnp.broadcast_to(value[None], (lax.axis_size(axes), *value.shape))
    return swapped(copies, axes)


def padded_to(value, size, axis):
    widths = [(0, 0)] * value.ndim
    widths[axis] = (0, size - value.shape[axis])
    return jnp.pad(value, widths)


def gathered_in_steps(own, axis):
    size = lax.axis_size(axis)

    def taken_from(value, away):
        return lax.ppermute(value, axis, [((i + away) % size, i) for i in range(size)])

    far = taken_from(own, 4)
    ahead = taken_from(own, 2)
    behind = taken_from(own, -2)
    odd_ahead = taken_from(jnp.concatenate([own, ahead]), 1)
    odd_behind = taken_from(jnp.concatenate([own, behind]), -1)
    return jnp.concatenate([own, far, ahead, behind, odd_ahead, odd_behind])


def with_neighbours(rows, blocks):
    width = rows.shape[1]
    main = rows.reshape(blocks, -1, width)
    nothing = jnp.zeros((1, width), rows.dtype)
    before = jnp.concatenate([nothing, main[:-1, -1]], axis=0)[:, None]
    after = jnp.concatenate([main[1:, 0], nothing], axis=0)[:, None]
    rest = jnp.zeros((blocks, TILE - 2, width), rows.dtype)
    return jnp.concatenate([main, before, after, rest], axis=1)


def split_in_two(value):
    high = lax.reduce_precision(value, 8, 7)
    return high, value - high


def split_in_three(value):
    first, rest = split_in_two(value)
    second, third = split_in_two(rest)
    return jnp.concatenate([first, second, third], axis=0).astype(jnp.bfloat16)


def side_by_side(gate_weight, up_weight):
    return jnp.concatenate(
        [padded_to(gate_weight, LANES, 1), padded_to(up_weight, LANES, 1)], axis=1
    ).astype(jnp.bfloat16)


def with_squares(product, squares, hidden):
    high, low = split_in_two(squares)
    column = lax.broadcasted_iota(jnp.int32, product.shape, product.ndim - 1)
    product = jnp.where(column == hidden, high, product)
    return jnp.where(column == hidden + 1, low, product)


def activated(total, features, hidden, params):
    rows = total.shape[0] - TILE
    square_sum = total[:, hidden : hidden + 1] + total[:, hidden + 1 : hidden + 2]
    rscale = lax.rsqrt(square_sum / features + norm_eps)
    gate = total[:, :LANES] * rscale * params[4]
    upward = total[:rows, LANES:] * rscale[:rows] * params[5]
    main = gate[:rows]
    before = jnp.concatenate([gate[rows : rows + 1], main[:-1]], axis=0)
    after = jnp.concatenate([main[1:], gate[rows + 1 : rows + 2]], axis=0)
    mixed = params[0] * before + params[1] * main + params[2] * after + params[3]
    return (jax.nn.silu(mixed) * upward).astype(jnp.bfloat16)


def own_params(conv_taps, conv_bias, gate_scale, up_scale):
    stacked = jnp.concatenate([conv_taps, conv_bias[None], gate_scale[None], up_scale[None]], axis=0)
    return padded_to(stacked, LANES, 1)


def both_layers(
    tokens,
    gate_weight,
    up_weight,
    down_weight,
    gate_scale,
    up_scale,
    down_scale,
    norm_gain,
    conv_taps,
    conv_bias,
):
    blocks_c, blocks_y, blocks_z = (lax.axis_size(a) for a in ("cb", "ra_1", "ra_0"))
    at_y, at_z = lax.axis_index("ra_1"), lax.axis_index("ra_0")
    length, width = tokens.shape
    hidden = gate_weight.shape[2]
    features = width * blocks_c
    block = length // blocks_y
    f32, bf16 = jnp.float32, jnp.bfloat16

    params_1 = own_params(conv_taps[1], conv_bias[1], gate_scale[1], up_scale[1])
    carried = padded_to(split_in_three(padded_to(params_1, TILE, 0)), width, 1)
    packed = jnp.concatenate(
        [
            gate_weight[1].T.astype(bf16),
            up_weight[1].T.astype(bf16),
            down_weight[1].astype(bf16),
            carried,
        ],
        axis=0,
    )
    packed = gathered_in_steps(packed[None], "ra_1")

    params_0 = own_params(conv_taps[0], conv_bias[0], gate_scale[0], up_scale[0])
    wide = tokens.astype(f32)
    squares = jnp.sum(wide * wide, axis=1, keepdims=True)
    operand = (wide * norm_gain[0]).astype(bf16)
    product = jnp.dot(
        operand, side_by_side(gate_weight[0], up_weight[0]), preferred_element_type=f32
    )
    product = with_squares(product, squares, hidden).astype(bf16)
    total = swapped(with_neighbours(product, blocks_c), "cb").astype(f32).sum(axis=0)
    inner = activated(total, features, hidden, params_0)
    inner = sent_to_all(inner, "cb").reshape(length, LANES)
    down_0 = padded_to(down_weight[0], LANES, 0).astype(bf16)
    term = jnp.dot(inner, down_0, preferred_element_type=f32).astype(bf16)

    halves = 2
    groups = blocks_z // halves
    share_rows, half = block // groups, width // halves
    term = term.reshape(blocks_y, groups, share_rows, halves, half).transpose(1, 3, 0, 2, 4)
    part = swapped(term.reshape(blocks_z, blocks_y * share_rows, half), "ra_0")
    part = part.astype(f32).sum(axis=0).astype(bf16)
    part = swapped(with_neighbours(part, blocks_y), "ra_1").astype(f32).sum(axis=0)
    group, column = at_z // halves, (at_z % halves) * half

    def residual_rows(block_at, row, count):
        start = jnp.clip(block_at, 0, blocks_y - 1) * block + group * share_rows + row
        rows = lax.dynamic_slice(tokens, (start, column), (count, half))
        inside = (block_at >= 0) & (block_at < blocks_y)
        return jnp.where(inside, rows, jnp.zeros_like(rows))

    own = jnp.concatenate(
        [
            residual_rows(at_y, 0, share_rows),
            residual_rows(at_y - 1, share_rows - 1, 1),
            residual_rows(at_y + 1, 0, 1),
            jnp.zeros((TILE - 2, half), bf16),
        ],
        axis=0,
    )
    scale = lax.dynamic_slice_in_dim(down_scale[0], column, half, 0)
    fresh = (residual_scale * own.astype(f32) + part * scale).astype(bf16)
    fresh = sent_to_all(fresh, "ra_0").reshape(groups, halves, share_rows + TILE, half)
    rows = fresh[:, :, :share_rows].transpose(0, 2, 1, 3).reshape(block, width)
    before = fresh[groups - 1, :, share_rows].reshape(1, width)
    after = fresh[0, :, share_rows + 1].reshape(1, width)
    hstate = jnp.concatenate([rows, before, after, jnp.zeros((TILE - 2, width), bf16)], axis=0)

    wide = hstate.astype(f32)
    squares = jnp.sum(wide * wide, axis=1, keepdims=True)
    operand = (wide * norm_gain[1]).astype(bf16)
    product = jnp.concatenate(
        [
            padded_to(
                jnp.einsum("td,ykd->ytk", operand, weight, preferred_element_type=f32), LANES, 2
            )
            for weight in (packed[:, :hidden], packed[:, hidden : 2 * hidden])
        ],
        axis=2,
    )
    product = with_squares(product, squares[None], hidden).astype(bf16)
    total = swapped(product, "cb").astype(f32).sum(axis=0)
    theirs = lax.dynamic_index_in_dim(packed, lax.axis_index("cb"), 0, keepdims=False)
    theirs = theirs[3 * hidden :, :LANES].astype(f32).reshape(3, TILE, LANES)
    theirs = theirs[0] + theirs[1] + theirs[2]
    inner = activated(total, features, hidden, theirs)
    inner = sent_to_all(inner, "cb")
    down_1 = packed[:, 2 * hidden : 3 * hidden]
    term = jnp.einsum("ytk,ykf->tf", inner[:, :, :hidden], down_1, preferred_element_type=f32)
    term = term.astype(bf16)
    share_rows = block // blocks_z
    part = swapped(term.reshape(blocks_z, share_rows, width), "ra_0").astype(f32).sum(axis=0)
    own = lax.dynamic_slice_in_dim(hstate, share_rows * at_z, share_rows, 0).astype(f32)
    fresh = (residual_scale * own + part * down_scale[1]).astype(bf16)
    fresh = sent_to_all(fresh, "ra_0").reshape(block, width)
    return sent_to_all(fresh, "ra_1").reshape(length, width)


def solution(mesh):
    split = Mesh(mesh.devices.reshape(16, 8, mesh.shape["cb"]), ("ra_0", "ra_1", "cb"))
    return jax.shard_map(
        both_layers,
        mesh=split,
        in_specs=(
            P(None, "cb"),
            P(None, "cb", RA),
            P(None, "cb", RA),
            P(None, RA, "cb"),
            P(None, RA),
            P(None, RA),
            P(None, "cb"),
            P(None, "cb"),
            P(None, None, RA),
            P(None, RA),
        ),
        out_specs=P(None, "cb"),
        check_vma=False,
    )
```

```python
import jax
import jax.numpy as jnp
from jax import lax
from jax.sharding import Mesh
from jax.sharding import PartitionSpec as P


RA = ("ra_0", "ra_1")
LANES = 128
TILE = 8

norm_eps = 1e-06
residual_scale = 0.25


def swapped(pieces, axes):
    return lax.all_to_all(pieces, axes, 0, 0, tiled=True)


def sent_to_all(value, axes):
    copies = jnp.broadcast_to(value[None], (lax.axis_size(axes), *value.shape))
    return swapped(copies, axes)


def padded_to(value, size, axis):
    widths = [(0, 0)] * value.ndim
    widths[axis] = (0, size - value.shape[axis])
    return jnp.pad(value, widths)


def gathered_in_steps(own, axis):
    size = lax.axis_size(axis)

    def taken_from(value, away):
        return lax.ppermute(value, axis, [((i + away) % size, i) for i in range(size)])

    far = taken_from(own, 4)
    ahead = taken_from(own, 2)
    behind = taken_from(own, -2)
    odd_ahead = taken_from(jnp.concatenate([own, ahead]), 1)
    odd_behind = taken_from(jnp.concatenate([own, behind]), -1)
    return jnp.concatenate([own, ahead, behind, odd_ahead, odd_behind, far])


def with_neighbours(rows, blocks):
    width = rows.shape[1]
    main = rows.reshape(blocks, -1, width)
    nothing = jnp.zeros((1, width), rows.dtype)
    before = jnp.concatenate([nothing, main[:-1, -1]], axis=0)[:, None]
    after = jnp.concatenate([main[1:, 0], nothing], axis=0)[:, None]
    rest = jnp.zeros((blocks, TILE - 2, width), rows.dtype)
    return jnp.concatenate([main, before, after, rest], axis=1)


def split_in_two(value):
    high = lax.reduce_precision(value, 8, 7)
    return high, value - high


def split_in_three(value):
    first, rest = split_in_two(value)
    second, third = split_in_two(rest)
    return jnp.concatenate([first, second, third], axis=0).astype(jnp.bfloat16)


def side_by_side(gate_weight, up_weight):
    return jnp.concatenate(
        [padded_to(gate_weight, LANES, 1), padded_to(up_weight, LANES, 1)], axis=1
    ).astype(jnp.bfloat16)


def with_squares(product, squares, hidden):
    high, low = split_in_two(squares)
    column = lax.broadcasted_iota(jnp.int32, product.shape, product.ndim - 1)
    product = jnp.where(column == hidden, high, product)
    return jnp.where(column == hidden + 1, low, product)


def activated(total, features, hidden, params):
    rows = total.shape[0] - TILE
    square_sum = total[:, hidden : hidden + 1] + total[:, hidden + 1 : hidden + 2]
    rscale = lax.rsqrt(square_sum / features + norm_eps)
    gate = total[:, :LANES] * rscale * params[4]
    upward = total[:rows, LANES:] * rscale[:rows] * params[5]
    main = gate[:rows]
    before = jnp.concatenate([gate[rows : rows + 1], main[:-1]], axis=0)
    after = jnp.concatenate([main[1:], gate[rows + 1 : rows + 2]], axis=0)
    mixed = params[0] * before + params[1] * main + params[2] * after + params[3]
    return (jax.nn.silu(mixed) * upward).astype(jnp.bfloat16)


def own_params(conv_taps, conv_bias, gate_scale, up_scale):
    stacked = jnp.concatenate([conv_taps, conv_bias[None], gate_scale[None], up_scale[None]], axis=0)
    return padded_to(stacked, LANES, 1)


def both_layers(
    tokens,
    gate_weight,
    up_weight,
    down_weight,
    gate_scale,
    up_scale,
    down_scale,
    norm_gain,
    conv_taps,
    conv_bias,
):
    blocks_c, blocks_y, blocks_z = (lax.axis_size(a) for a in ("cb", "ra_1", "ra_0"))
    at_y, at_z = lax.axis_index("ra_1"), lax.axis_index("ra_0")
    length, width = tokens.shape
    hidden = gate_weight.shape[2]
    features = width * blocks_c
    block = length // blocks_y
    f32, bf16 = jnp.float32, jnp.bfloat16

    params_1 = own_params(conv_taps[1], conv_bias[1], gate_scale[1], up_scale[1])
    carried = padded_to(split_in_three(padded_to(params_1, TILE, 0)), width, 1)
    packed = jnp.concatenate(
        [
            gate_weight[1].T.astype(bf16),
            up_weight[1].T.astype(bf16),
            down_weight[1].astype(bf16),
            carried,
        ],
        axis=0,
    )
    packed = gathered_in_steps(packed[None], "ra_1")

    params_0 = own_params(conv_taps[0], conv_bias[0], gate_scale[0], up_scale[0])
    wide = tokens.astype(f32)
    squares = jnp.sum(wide * wide, axis=1, keepdims=True)
    operand = (wide * norm_gain[0]).astype(bf16)
    product = jnp.dot(
        operand, side_by_side(gate_weight[0], up_weight[0]), preferred_element_type=f32
    )
    product = with_squares(product, squares, hidden).astype(bf16)
    total = swapped(with_neighbours(product, blocks_c), "cb").astype(f32).sum(axis=0)
    inner = activated(total, features, hidden, params_0)
    inner = sent_to_all(inner, "cb").reshape(length, LANES)
    down_0 = padded_to(down_weight[0], LANES, 0).astype(bf16)
    term = jnp.dot(inner, down_0, preferred_element_type=f32).astype(bf16)
    part = swapped(with_neighbours(term, blocks_y), "ra_1").astype(f32).sum(axis=0)
    share_rows = TILE
    part = padded_to(part.astype(bf16), share_rows * blocks_z, 0)
    part = swapped(part.reshape(blocks_z, share_rows, width), "ra_0").astype(f32).sum(axis=0)

    start = block * at_y
    mains = block // share_rows
    own = lax.dynamic_slice_in_dim(tokens, start + share_rows * jnp.minimum(at_z, mains - 1), share_rows, 0)
    before = lax.dynamic_slice_in_dim(tokens, jnp.maximum(start - 1, 0), 1, 0)
    after = lax.dynamic_slice_in_dim(tokens, jnp.minimum(start + block, length - 1), 1, 0)
    row = lax.broadcasted_iota(jnp.int32, (share_rows, 1), 0)
    edge = jnp.where((row == 0) & (at_y > 0), before, jnp.zeros_like(before))
    edge = jnp.where((row == 1) & (at_y < blocks_y - 1), after, edge)
    own = jnp.where(at_z < mains, own, jnp.where(at_z == mains, edge, jnp.zeros_like(edge)))
    fresh = (residual_scale * own.astype(f32) + part * down_scale[0]).astype(bf16)
    hstate = sent_to_all(fresh, "ra_0").reshape(blocks_z * share_rows, width)[: block + TILE]

    wide = hstate.astype(f32)
    squares = jnp.sum(wide * wide, axis=1, keepdims=True)
    operand = (wide * norm_gain[1]).astype(bf16)
    product = jnp.concatenate(
        [
            padded_to(
                jnp.einsum("td,ykd->ytk", operand, weight, preferred_element_type=f32), LANES, 2
            )
            for weight in (packed[:, :hidden], packed[:, hidden : 2 * hidden])
        ],
        axis=2,
    )
    product = with_squares(product, squares[None], hidden).astype(bf16)
    total = swapped(product, "cb").astype(f32).sum(axis=0)
    theirs = lax.dynamic_index_in_dim(packed, lax.axis_index("cb"), 0, keepdims=False)
    theirs = theirs[3 * hidden :, :LANES].astype(f32).reshape(3, TILE, LANES)
    theirs = theirs[0] + theirs[1] + theirs[2]
    inner = activated(total, features, hidden, theirs)
    inner = sent_to_all(inner, "cb")
    down_1 = packed[:, 2 * hidden : 3 * hidden]
    term = jnp.einsum("ytk,ykf->tf", inner[:, :, :hidden], down_1, preferred_element_type=f32)
    term = term.astype(bf16)
    share_rows = block // blocks_z
    part = swapped(term.reshape(blocks_z, share_rows, width), "ra_0").astype(f32).sum(axis=0)
    own = lax.dynamic_slice_in_dim(hstate, share_rows * at_z, share_rows, 0).astype(f32)
    fresh = (residual_scale * own + part * down_scale[1]).astype(bf16)
    fresh = sent_to_all(fresh, "ra_0").reshape(block, width)
    return sent_to_all(fresh, "ra_1").reshape(length, width)


def solution(mesh):
    split = Mesh(mesh.devices.reshape(16, 8, mesh.shape["cb"]), ("ra_0", "ra_1", "cb"))
    return jax.shard_map(
        both_layers,
        mesh=split,
        in_specs=(
            P(None, "cb"),
            P(None, "cb", RA),
            P(None, "cb", RA),
            P(None, RA, "cb"),
            P(None, RA),
            P(None, RA),
            P(None, "cb"),
            P(None, "cb"),
            P(None, None, RA),
            P(None, RA),
        ),
        out_specs=P(None, "cb"),
        check_vma=False,
    )
```

```python
import jax
import jax.numpy as jnp
from jax import lax
from jax.experimental import pallas as pl
from jax.sharding import Mesh
from jax.sharding import PartitionSpec as P


RA = ("ra_0", "ra_1")
LANES = 128
TILE = 8

norm_eps = 1e-06
residual_scale = 0.25


def swapped(pieces, axes):
    return lax.all_to_all(pieces, axes, 0, 0, tiled=True)


def sent_to_all(value, axes):
    copies = jnp.broadcast_to(value[None], (lax.axis_size(axes), *value.shape))
    return swapped(copies, axes)


def padded_to(value, size, axis):
    widths = [(0, 0)] * value.ndim
    widths[axis] = (0, size - value.shape[axis])
    return jnp.pad(value, widths)


def gathered_in_steps(own, axis):
    size = lax.axis_size(axis)

    def taken_from(value, away):
        return lax.ppermute(value, axis, [((i + away) % size, i) for i in range(size)])

    far = taken_from(own, 4)
    ahead = taken_from(own, 2)
    behind = taken_from(own, -2)
    odd_ahead = taken_from(jnp.concatenate([own, ahead]), 1)
    odd_behind = taken_from(jnp.concatenate([own, behind]), -1)
    return jnp.concatenate([own, ahead, behind, odd_ahead, odd_behind, far])


def with_neighbours(rows, blocks):
    width = rows.shape[1]
    main = rows.reshape(blocks, -1, width)
    nothing = jnp.zeros((1, width), rows.dtype)
    before = jnp.concatenate([nothing, main[:-1, -1]], axis=0)[:, None]
    after = jnp.concatenate([main[1:, 0], nothing], axis=0)[:, None]
    rest = jnp.zeros((blocks, TILE - 2, width), rows.dtype)
    return jnp.concatenate([main, before, after, rest], axis=1)


def split_in_two(value):
    high = lax.reduce_precision(value, 8, 7)
    return high, value - high


def split_in_three(value):
    first, rest = split_in_two(value)
    second, third = split_in_two(rest)
    return jnp.concatenate([first, second, third], axis=0).astype(jnp.bfloat16)


def with_squares(product, squares, hidden):
    high, low = split_in_two(squares)
    column = lax.broadcasted_iota(jnp.int32, product.shape, product.ndim - 1)
    product = jnp.where(column == hidden, high, product)
    return jnp.where(column == hidden + 1, low, product)


def first_products(tokens, gain, gate_weight, up_weight, blocks):
    length, width = tokens.shape
    hidden = gate_weight.shape[1]
    block = length // blocks

    def kernel(tokens_ref, gain_ref, gate_ref, up_ref, out_ref):
        wide = tokens_ref[...].astype(jnp.float32)
        squares = jnp.sum(wide * wide, axis=1, keepdims=True)
        operand = (wide * gain_ref[0:1]).astype(jnp.bfloat16)
        rest = jnp.zeros((LANES - hidden, width), jnp.float32)
        weight = jnp.concatenate([gate_ref[0], rest, up_ref[0], rest], axis=0).astype(jnp.bfloat16)
        product = lax.dot_general(
            operand, weight, (((1,), (1,)), ((), ())), preferred_element_type=jnp.float32
        )
        high = squares.astype(jnp.bfloat16).astype(jnp.float32)
        column = lax.broadcasted_iota(jnp.int32, product.shape, 1)
        product = jnp.where(column == hidden, high, product)
        product = jnp.where(column == hidden + 1, squares - high, product)
        row = lax.broadcasted_iota(jnp.int32, (TILE, 2 * LANES), 0)
        nothing = jnp.zeros((TILE, 2 * LANES), jnp.float32)
        for j in range(blocks):
            start = j * block
            edge = nothing
            if j > 0:
                edge = jnp.where(row == 0, product[start - 1 : start], edge)
            if j < blocks - 1:
                edge = jnp.where(row == 1, product[start + block : start + block + 1], edge)
            out_ref[j] = jnp.concatenate([product[start : start + block], edge], axis=0).astype(
                jnp.bfloat16
            )

    shape = (blocks, block + TILE, 2 * LANES)
    weight_block = pl.BlockSpec((1, hidden, width), lambda i: (0, 0, 0))
    return pl.pallas_call(
        kernel,
        grid=(1,),
        in_specs=[
            pl.BlockSpec((length, width), lambda i: (0, 0)),
            pl.BlockSpec(gain.shape, lambda i: (0, 0)),
            weight_block,
            weight_block,
        ],
        out_specs=pl.BlockSpec(shape, lambda i: (0, 0, 0)),
        out_shape=jax.ShapeDtypeStruct(shape, jnp.bfloat16),
    )(tokens, gain, gate_weight, up_weight)


def activated(total, features, hidden, params):
    rows = total.shape[0] - TILE
    square_sum = total[:, hidden : hidden + 1] + total[:, hidden + 1 : hidden + 2]
    rscale = lax.rsqrt(square_sum / features + norm_eps)
    gate = total[:, :LANES] * rscale * params[4]
    upward = total[:rows, LANES:] * rscale[:rows] * params[5]
    main = gate[:rows]
    before = jnp.concatenate([gate[rows : rows + 1], main[:-1]], axis=0)
    after = jnp.concatenate([main[1:], gate[rows + 1 : rows + 2]], axis=0)
    mixed = params[0] * before + params[1] * main + params[2] * after + params[3]
    return (jax.nn.silu(mixed) * upward).astype(jnp.bfloat16)


def own_params(conv_taps, conv_bias, gate_scale, up_scale):
    stacked = jnp.concatenate([conv_taps, conv_bias[None], gate_scale[None], up_scale[None]], axis=0)
    return padded_to(stacked, LANES, 1)


def both_layers(
    tokens,
    gate_weight,
    up_weight,
    down_weight,
    gate_scale,
    up_scale,
    down_scale,
    norm_gain,
    conv_taps,
    conv_bias,
):
    blocks_c, blocks_y, blocks_z = (lax.axis_size(a) for a in ("cb", "ra_1", "ra_0"))
    at_y, at_z = lax.axis_index("ra_1"), lax.axis_index("ra_0")
    length, width = tokens.shape
    hidden = gate_weight.shape[2]
    features = width * blocks_c
    block = length // blocks_y
    f32, bf16 = jnp.float32, jnp.bfloat16

    params_1 = own_params(conv_taps[1], conv_bias[1], gate_scale[1], up_scale[1])
    carried = padded_to(split_in_three(padded_to(params_1, TILE, 0)), width, 1)
    packed = jnp.concatenate(
        [
            gate_weight[1].T.astype(bf16),
            up_weight[1].T.astype(bf16),
            down_weight[1].astype(bf16),
            carried,
        ],
        axis=0,
    )
    packed = gathered_in_steps(packed[None], "ra_1")

    params_0 = own_params(conv_taps[0], conv_bias[0], gate_scale[0], up_scale[0])
    product = first_products(
        tokens,
        norm_gain,
        jnp.swapaxes(gate_weight, 1, 2),
        jnp.swapaxes(up_weight, 1, 2),
        blocks_c,
    )
    total = swapped(product, "cb").astype(f32).sum(axis=0)
    inner = activated(total, features, hidden, params_0)
    inner = sent_to_all(inner, "cb").reshape(length, LANES)
    down_0 = padded_to(down_weight[0], LANES, 0).astype(bf16)
    term = jnp.dot(inner, down_0, preferred_element_type=f32).astype(bf16)
    part = swapped(with_neighbours(term, blocks_y), "ra_1").astype(f32).sum(axis=0)
    share_rows = TILE
    part = padded_to(part.astype(bf16), share_rows * blocks_z, 0)
    part = swapped(part.reshape(blocks_z, share_rows, width), "ra_0").astype(f32).sum(axis=0)

    start = block * at_y
    mains = block // share_rows
    own = lax.dynamic_slice_in_dim(tokens, start + share_rows * jnp.minimum(at_z, mains - 1), share_rows, 0)
    before = lax.dynamic_slice_in_dim(tokens, jnp.maximum(start - 1, 0), 1, 0)
    after = lax.dynamic_slice_in_dim(tokens, jnp.minimum(start + block, length - 1), 1, 0)
    row = lax.broadcasted_iota(jnp.int32, (share_rows, 1), 0)
    edge = jnp.where((row == 0) & (at_y > 0), before, jnp.zeros_like(before))
    edge = jnp.where((row == 1) & (at_y < blocks_y - 1), after, edge)
    own = jnp.where(at_z < mains, own, jnp.where(at_z == mains, edge, jnp.zeros_like(edge)))
    fresh = (residual_scale * own.astype(f32) + part * down_scale[0]).astype(bf16)
    hstate = sent_to_all(fresh, "ra_0").reshape(blocks_z * share_rows, width)[: block + TILE]

    wide = hstate.astype(f32)
    squares = jnp.sum(wide * wide, axis=1, keepdims=True)
    operand = (wide * norm_gain[1]).astype(bf16)
    product = jnp.concatenate(
        [
            padded_to(
                jnp.einsum("td,ykd->ytk", operand, weight, preferred_element_type=f32), LANES, 2
            )
            for weight in (packed[:, :hidden], packed[:, hidden : 2 * hidden])
        ],
        axis=2,
    )
    product = with_squares(product, squares[None], hidden).astype(bf16)
    total = swapped(product, "cb").astype(f32).sum(axis=0)
    theirs = lax.dynamic_index_in_dim(packed, lax.axis_index("cb"), 0, keepdims=False)
    theirs = theirs[3 * hidden :, :LANES].astype(f32).reshape(3, TILE, LANES)
    theirs = theirs[0] + theirs[1] + theirs[2]
    inner = activated(total, features, hidden, theirs)
    inner = sent_to_all(inner, "cb")
    down_1 = packed[:, 2 * hidden : 3 * hidden]
    term = jnp.einsum("ytk,ykf->tf", inner[:, :, :hidden], down_1, preferred_element_type=f32)
    term = term.astype(bf16)
    share_rows = block // blocks_z
    part = swapped(term.reshape(blocks_z, share_rows, width), "ra_0").astype(f32).sum(axis=0)
    own = lax.dynamic_slice_in_dim(hstate, share_rows * at_z, share_rows, 0).astype(f32)
    fresh = (residual_scale * own + part * down_scale[1]).astype(bf16)
    fresh = sent_to_all(fresh, "ra_0").reshape(block, width)
    return sent_to_all(fresh, "ra_1").reshape(length, width)


def solution(mesh):
    split = Mesh(mesh.devices.reshape(16, 8, mesh.shape["cb"]), ("ra_0", "ra_1", "cb"))
    return jax.shard_map(
        both_layers,
        mesh=split,
        in_specs=(
            P(None, "cb"),
            P(None, "cb", RA),
            P(None, "cb", RA),
            P(None, RA, "cb"),
            P(None, RA),
            P(None, RA),
            P(None, "cb"),
            P(None, "cb"),
            P(None, None, RA),
            P(None, RA),
        ),
        out_specs=P(None, "cb"),
        check_vma=False,
    )
```

```python
import jax
import jax.numpy as jnp
from jax import lax
from jax.experimental import pallas as pl
from jax.sharding import Mesh
from jax.sharding import PartitionSpec as P


RA = ("ra_0", "ra_1")
LANES = 128
TILE = 8

norm_eps = 1e-06
residual_scale = 0.25


def swapped(pieces, axes):
    return lax.all_to_all(pieces, axes, 0, 0, tiled=True)


def sent_to_all(value, axes):
    copies = jnp.broadcast_to(value[None], (lax.axis_size(axes), *value.shape))
    return swapped(copies, axes)


def padded_to(value, size, axis):
    widths = [(0, 0)] * value.ndim
    widths[axis] = (0, size - value.shape[axis])
    return jnp.pad(value, widths)


def gathered_in_steps(own, axis):
    size = lax.axis_size(axis)

    def taken_from(value, away):
        return lax.ppermute(value, axis, [((i + away) % size, i) for i in range(size)])

    far = taken_from(own, 4)
    ahead = taken_from(own, 2)
    behind = taken_from(own, -2)
    odd_ahead = taken_from(jnp.concatenate([own, ahead]), 1)
    odd_behind = taken_from(jnp.concatenate([own, behind]), -1)
    return jnp.concatenate([own, ahead, behind, far, odd_ahead, odd_behind])


def with_neighbours(rows, blocks):
    width = rows.shape[1]
    main = rows.reshape(blocks, -1, width)
    nothing = jnp.zeros((1, width), rows.dtype)
    before = jnp.concatenate([nothing, main[:-1, -1]], axis=0)[:, None]
    after = jnp.concatenate([main[1:, 0], nothing], axis=0)[:, None]
    rest = jnp.zeros((blocks, TILE - 2, width), rows.dtype)
    return jnp.concatenate([main, before, after, rest], axis=1)


def split_in_two(value):
    high = lax.reduce_precision(value, 8, 7)
    return high, value - high


def split_in_three(value):
    first, rest = split_in_two(value)
    second, third = split_in_two(rest)
    return jnp.concatenate([first, second, third], axis=0).astype(jnp.bfloat16)


def with_squares(product, squares, hidden):
    high, low = split_in_two(squares)
    column = lax.broadcasted_iota(jnp.int32, product.shape, product.ndim - 1)
    product = jnp.where(column == hidden, high, product)
    return jnp.where(column == hidden + 1, low, product)


def first_products(tokens, gain, gate_weight, up_weight, blocks):
    length, width = tokens.shape
    hidden = gate_weight.shape[1]
    block = length // blocks

    def kernel(tokens_ref, gain_ref, gate_ref, up_ref, out_ref):
        wide = tokens_ref[...].astype(jnp.float32)
        squares = jnp.sum(wide * wide, axis=1, keepdims=True)
        operand = (wide * gain_ref[0:1]).astype(jnp.bfloat16)
        rest = jnp.zeros((LANES - hidden, width), jnp.float32)
        weight = jnp.concatenate([gate_ref[0], rest, up_ref[0], rest], axis=0).astype(jnp.bfloat16)
        product = lax.dot_general(
            operand, weight, (((1,), (1,)), ((), ())), preferred_element_type=jnp.float32
        )
        high = squares.astype(jnp.bfloat16).astype(jnp.float32)
        column = lax.broadcasted_iota(jnp.int32, product.shape, 1)
        product = jnp.where(column == hidden, high, product)
        product = jnp.where(column == hidden + 1, squares - high, product)
        row = lax.broadcasted_iota(jnp.int32, (TILE, 2 * LANES), 0)
        nothing = jnp.zeros((TILE, 2 * LANES), jnp.float32)
        for j in range(blocks):
            start = j * block
            edge = nothing
            if j > 0:
                edge = jnp.where(row == 0, product[start - 1 : start], edge)
            if j < blocks - 1:
                edge = jnp.where(row == 1, product[start + block : start + block + 1], edge)
            out_ref[j] = jnp.concatenate([product[start : start + block], edge], axis=0).astype(
                jnp.bfloat16
            )

    shape = (blocks, block + TILE, 2 * LANES)
    weight_block = pl.BlockSpec((1, hidden, width), lambda i: (0, 0, 0))
    return pl.pallas_call(
        kernel,
        grid=(1,),
        in_specs=[
            pl.BlockSpec((length, width), lambda i: (0, 0)),
            pl.BlockSpec(gain.shape, lambda i: (0, 0)),
            weight_block,
            weight_block,
        ],
        out_specs=pl.BlockSpec(shape, lambda i: (0, 0, 0)),
        out_shape=jax.ShapeDtypeStruct(shape, jnp.bfloat16),
    )(tokens, gain, gate_weight, up_weight)


def activated(total, features, hidden, params):
    rows = total.shape[0] - TILE
    square_sum = total[:, hidden : hidden + 1] + total[:, hidden + 1 : hidden + 2]
    rscale = lax.rsqrt(square_sum / features + norm_eps)
    gate = total[:, :LANES] * rscale * params[4]
    upward = total[:rows, LANES:] * rscale[:rows] * params[5]
    main = gate[:rows]
    before = jnp.concatenate([gate[rows : rows + 1], main[:-1]], axis=0)
    after = jnp.concatenate([main[1:], gate[rows + 1 : rows + 2]], axis=0)
    mixed = params[0] * before + params[1] * main + params[2] * after + params[3]
    return (jax.nn.silu(mixed) * upward).astype(jnp.bfloat16)


def own_params(conv_taps, conv_bias, gate_scale, up_scale):
    stacked = jnp.concatenate([conv_taps, conv_bias[None], gate_scale[None], up_scale[None]], axis=0)
    return padded_to(stacked, LANES, 1)


def both_layers(
    tokens,
    gate_weight,
    up_weight,
    down_weight,
    gate_scale,
    up_scale,
    down_scale,
    norm_gain,
    conv_taps,
    conv_bias,
):
    blocks_c, blocks_y, blocks_z = (lax.axis_size(a) for a in ("cb", "ra_1", "ra_0"))
    at_y, at_z = lax.axis_index("ra_1"), lax.axis_index("ra_0")
    length, width = tokens.shape
    hidden = gate_weight.shape[2]
    features = width * blocks_c
    block = length // blocks_y
    f32, bf16 = jnp.float32, jnp.bfloat16

    params_1 = own_params(conv_taps[1], conv_bias[1], gate_scale[1], up_scale[1])
    carried = padded_to(split_in_three(padded_to(params_1, TILE, 0)), width, 1)
    packed = jnp.concatenate(
        [
            gate_weight[1].T.astype(bf16),
            up_weight[1].T.astype(bf16),
            down_weight[1].astype(bf16),
            carried,
        ],
        axis=0,
    )
    packed = gathered_in_steps(packed[None], "ra_1")

    params_0 = own_params(conv_taps[0], conv_bias[0], gate_scale[0], up_scale[0])
    product = first_products(
        tokens,
        norm_gain,
        jnp.swapaxes(gate_weight, 1, 2),
        jnp.swapaxes(up_weight, 1, 2),
        blocks_c,
    )
    total = swapped(product, "cb").astype(f32).sum(axis=0)
    inner = activated(total, features, hidden, params_0)
    inner = sent_to_all(inner, "cb").reshape(length, LANES)
    down_0 = padded_to(down_weight[0], LANES, 0).astype(bf16)
    term = jnp.dot(inner, down_0, preferred_element_type=f32).astype(bf16)

    halves = 2
    groups = blocks_z // halves
    share_rows, half = block // groups, width // halves
    term = term.reshape(blocks_y, groups, share_rows, halves, half).transpose(1, 3, 0, 2, 4)
    part = swapped(term.reshape(blocks_z, blocks_y * share_rows, half), "ra_0")
    part = part.astype(f32).sum(axis=0).astype(bf16)
    part = swapped(with_neighbours(part, blocks_y), "ra_1").astype(f32).sum(axis=0)
    group, column = at_z // halves, (at_z % halves) * half

    def residual_rows(block_at, row, count):
        start = jnp.clip(block_at, 0, blocks_y - 1) * block + group * share_rows + row
        rows = lax.dynamic_slice(tokens, (start, column), (count, half))
        inside = (block_at >= 0) & (block_at < blocks_y)
        return jnp.where(inside, rows, jnp.zeros_like(rows))

    own = jnp.concatenate(
        [
            residual_rows(at_y, 0, share_rows),
            residual_rows(at_y - 1, share_rows - 1, 1),
            residual_rows(at_y + 1, 0, 1),
            jnp.zeros((TILE - 2, half), bf16),
        ],
        axis=0,
    )
    scale = lax.dynamic_slice_in_dim(down_scale[0], column, half, 0)
    fresh = (residual_scale * own.astype(f32) + part * scale).astype(bf16)
    fresh = sent_to_all(fresh, "ra_0").reshape(groups, halves, share_rows + TILE, half)
    rows = fresh[:, :, :share_rows].transpose(0, 2, 1, 3).reshape(block, width)
    before = fresh[groups - 1, :, share_rows].reshape(1, width)
    after = fresh[0, :, share_rows + 1].reshape(1, width)
    hstate = jnp.concatenate([rows, before, after, jnp.zeros((TILE - 2, width), bf16)], axis=0)

    wide = hstate.astype(f32)
    squares = jnp.sum(wide * wide, axis=1, keepdims=True)
    operand = (wide * norm_gain[1]).astype(bf16)
    product = jnp.concatenate(
        [
            padded_to(
                jnp.einsum("td,ykd->ytk", operand, weight, preferred_element_type=f32), LANES, 2
            )
            for weight in (packed[:, :hidden], packed[:, hidden : 2 * hidden])
        ],
        axis=2,
    )
    product = with_squares(product, squares[None], hidden).astype(bf16)
    total = swapped(product, "cb").astype(f32).sum(axis=0)
    theirs = lax.dynamic_index_in_dim(packed, lax.axis_index("cb"), 0, keepdims=False)
    theirs = theirs[3 * hidden :, :LANES].astype(f32).reshape(3, TILE, LANES)
    theirs = theirs[0] + theirs[1] + theirs[2]
    inner = activated(total, features, hidden, theirs)
    inner = sent_to_all(inner, "cb")
    down_1 = packed[:, 2 * hidden : 3 * hidden]
    term = jnp.einsum("ytk,ykf->tf", inner[:, :, :hidden], down_1, preferred_element_type=f32)
    term = term.astype(bf16)
    share_rows = block // blocks_z
    part = swapped(term.reshape(blocks_z, share_rows, width), "ra_0").astype(f32).sum(axis=0)
    own = lax.dynamic_slice_in_dim(hstate, share_rows * at_z, share_rows, 0).astype(f32)
    fresh = (residual_scale * own + part * down_scale[1]).astype(bf16)
    fresh = sent_to_all(fresh, "ra_0").reshape(block, width)
    return sent_to_all(fresh, "ra_1").reshape(length, width)


def solution(mesh):
    split = Mesh(mesh.devices.reshape(16, 8, mesh.shape["cb"]), ("ra_0", "ra_1", "cb"))
    return jax.shard_map(
        both_layers,
        mesh=split,
        in_specs=(
            P(None, "cb"),
            P(None, "cb", RA),
            P(None, "cb", RA),
            P(None, RA, "cb"),
            P(None, RA),
            P(None, RA),
            P(None, "cb"),
            P(None, "cb"),
            P(None, None, RA),
            P(None, RA),
        ),
        out_specs=P(None, "cb"),
        check_vma=False,
    )
```

```python
import jax
import jax.numpy as jnp
from jax import lax
from jax.experimental import pallas as pl
from jax.sharding import Mesh
from jax.sharding import PartitionSpec as P


RA = ("ra_0", "ra_1")
LANES = 128
TILE = 8

norm_eps = 1e-06
residual_scale = 0.25


def swapped(pieces, axes):
    return lax.all_to_all(pieces, axes, 0, 0, tiled=True)


def sent_to_all(value, axes):
    copies = jnp.broadcast_to(value[None], (lax.axis_size(axes), *value.shape))
    return swapped(copies, axes)


def padded_to(value, size, axis):
    widths = [(0, 0)] * value.ndim
    widths[axis] = (0, size - value.shape[axis])
    return jnp.pad(value, widths)


def gathered_in_steps(own, axis):
    size = lax.axis_size(axis)

    def taken_from(value, away):
        return lax.ppermute(value, axis, [((i + away) % size, i) for i in range(size)])

    far = taken_from(own, 4)
    ahead = taken_from(own, 2)
    behind = taken_from(own, -2)
    odd_ahead = taken_from(jnp.concatenate([own, ahead]), 1)
    odd_behind = taken_from(jnp.concatenate([own, behind]), -1)
    return jnp.concatenate([own, ahead, behind, far, odd_ahead, odd_behind])


def with_neighbours(rows, blocks):
    width = rows.shape[1]
    main = rows.reshape(blocks, -1, width)
    nothing = jnp.zeros((1, width), rows.dtype)
    before = jnp.concatenate([nothing, main[:-1, -1]], axis=0)[:, None]
    after = jnp.concatenate([main[1:, 0], nothing], axis=0)[:, None]
    rest = jnp.zeros((blocks, TILE - 2, width), rows.dtype)
    return jnp.concatenate([main, before, after, rest], axis=1)


def split_in_two(value):
    high = lax.reduce_precision(value, 8, 7)
    return high, value - high


def split_in_three(value):
    first, rest = split_in_two(value)
    second, third = split_in_two(rest)
    return tuple(part.astype(jnp.bfloat16) for part in (first, second, third))


def with_squares(product, squares, hidden):
    high, low = split_in_two(squares)
    column = lax.broadcasted_iota(jnp.int32, product.shape, product.ndim - 1)
    product = jnp.where(column == hidden, high, product)
    return jnp.where(column == hidden + 1, low, product)


def first_products(tokens, gain, gate_weight, up_weight, blocks):
    length, width = tokens.shape
    hidden = gate_weight.shape[1]
    block = length // blocks

    def kernel(tokens_ref, gain_ref, gate_ref, up_ref, out_ref):
        wide = tokens_ref[...].astype(jnp.float32)
        squares = jnp.sum(wide * wide, axis=1, keepdims=True)
        operand = (wide * gain_ref[0:1]).astype(jnp.bfloat16)
        rest = jnp.zeros((LANES - hidden, width), jnp.float32)
        weight = jnp.concatenate([gate_ref[0], rest, up_ref[0], rest], axis=0).astype(jnp.bfloat16)
        product = lax.dot_general(
            operand, weight, (((1,), (1,)), ((), ())), preferred_element_type=jnp.float32
        )
        high = squares.astype(jnp.bfloat16).astype(jnp.float32)
        column = lax.broadcasted_iota(jnp.int32, product.shape, 1)
        product = jnp.where(column == hidden, high, product)
        product = jnp.where(column == hidden + 1, squares - high, product)
        row = lax.broadcasted_iota(jnp.int32, (TILE, 2 * LANES), 0)
        nothing = jnp.zeros((TILE, 2 * LANES), jnp.float32)
        for j in range(blocks):
            start = j * block
            edge = nothing
            if j > 0:
                edge = jnp.where(row == 0, product[start - 1 : start], edge)
            if j < blocks - 1:
                edge = jnp.where(row == 1, product[start + block : start + block + 1], edge)
            out_ref[j] = jnp.concatenate([product[start : start + block], edge], axis=0).astype(
                jnp.bfloat16
            )

    shape = (blocks, block + TILE, 2 * LANES)
    weight_block = pl.BlockSpec((1, hidden, width), lambda i: (0, 0, 0))
    return pl.pallas_call(
        kernel,
        grid=(1,),
        in_specs=[
            pl.BlockSpec((length, width), lambda i: (0, 0)),
            pl.BlockSpec(gain.shape, lambda i: (0, 0)),
            weight_block,
            weight_block,
        ],
        out_specs=pl.BlockSpec(shape, lambda i: (0, 0, 0)),
        out_shape=jax.ShapeDtypeStruct(shape, jnp.bfloat16),
    )(tokens, gain, gate_weight, up_weight)


def activated(total, features, hidden, up_at, params):
    rows = total.shape[0] - TILE
    square_sum = total[:, hidden : hidden + 1] + total[:, hidden + 1 : hidden + 2]
    rscale = lax.rsqrt(square_sum / features + norm_eps)
    gate = total[:, :LANES] * rscale * params[4]
    upward = total[:rows, up_at : up_at + LANES] * rscale[:rows] * params[5]
    main = gate[:rows]
    before = jnp.concatenate([gate[rows : rows + 1], main[:-1]], axis=0)
    after = jnp.concatenate([main[1:], gate[rows + 1 : rows + 2]], axis=0)
    mixed = params[0] * before + params[1] * main + params[2] * after + params[3]
    return (jax.nn.silu(mixed) * upward).astype(jnp.bfloat16)


def own_params(conv_taps, conv_bias, gate_scale, up_scale):
    stacked = jnp.concatenate([conv_taps, conv_bias[None], gate_scale[None], up_scale[None]], axis=0)
    return padded_to(stacked, LANES, 1)


def both_layers(
    tokens,
    gate_weight,
    up_weight,
    down_weight,
    gate_scale,
    up_scale,
    down_scale,
    norm_gain,
    conv_taps,
    conv_bias,
):
    blocks_c, blocks_y, blocks_z = (lax.axis_size(a) for a in ("cb", "ra_1", "ra_0"))
    at_y, at_z = lax.axis_index("ra_1"), lax.axis_index("ra_0")
    length, width = tokens.shape
    hidden = gate_weight.shape[2]
    features = width * blocks_c
    block = length // blocks_y
    f32, bf16 = jnp.float32, jnp.bfloat16

    params_1 = own_params(conv_taps[1], conv_bias[1], gate_scale[1], up_scale[1])
    carried = split_in_three(padded_to(padded_to(params_1, TILE, 0), width, 1))
    packed = jnp.concatenate(
        [
            gate_weight[1].T.astype(bf16),
            carried[0],
            up_weight[1].T.astype(bf16),
            carried[1],
            carried[2],
            down_weight[1].astype(bf16),
        ],
        axis=0,
    )
    up_at = hidden + TILE
    down_at = 2 * hidden + 3 * TILE
    packed = gathered_in_steps(packed[None], "ra_1")

    params_0 = own_params(conv_taps[0], conv_bias[0], gate_scale[0], up_scale[0])
    product = first_products(
        tokens,
        norm_gain,
        jnp.swapaxes(gate_weight, 1, 2),
        jnp.swapaxes(up_weight, 1, 2),
        blocks_c,
    )
    total = swapped(product, "cb").astype(f32).sum(axis=0)
    inner = activated(total, features, hidden, LANES, params_0)
    inner = sent_to_all(inner, "cb").reshape(length, LANES)
    down_0 = padded_to(down_weight[0], LANES, 0).astype(bf16)
    term = jnp.dot(inner, down_0, preferred_element_type=f32).astype(bf16)

    halves = 2
    groups = blocks_z // halves
    share_rows, half = block // groups, width // halves
    term = term.reshape(blocks_y, groups, share_rows, halves, half).transpose(1, 3, 0, 2, 4)
    part = swapped(term.reshape(blocks_z, blocks_y * share_rows, half), "ra_0")
    part = part.astype(f32).sum(axis=0).astype(bf16)
    part = swapped(with_neighbours(part, blocks_y), "ra_1").astype(f32).sum(axis=0)
    group, column = at_z // halves, (at_z % halves) * half

    def residual_rows(block_at, row, count):
        start = jnp.clip(block_at, 0, blocks_y - 1) * block + group * share_rows + row
        rows = lax.dynamic_slice(tokens, (start, column), (count, half))
        inside = (block_at >= 0) & (block_at < blocks_y)
        return jnp.where(inside, rows, jnp.zeros_like(rows))

    own = jnp.concatenate(
        [
            residual_rows(at_y, 0, share_rows),
            residual_rows(at_y - 1, share_rows - 1, 1),
            residual_rows(at_y + 1, 0, 1),
            jnp.zeros((TILE - 2, half), bf16),
        ],
        axis=0,
    )
    scale = lax.dynamic_slice_in_dim(down_scale[0], column, half, 0)
    fresh = (residual_scale * own.astype(f32) + part * scale).astype(bf16)
    fresh = sent_to_all(fresh, "ra_0").reshape(groups, halves, share_rows + TILE, half)
    rows = fresh[:, :, :share_rows].transpose(0, 2, 1, 3).reshape(block, width)
    before = fresh[groups - 1, :, share_rows].reshape(1, width)
    after = fresh[0, :, share_rows + 1].reshape(1, width)
    hstate = jnp.concatenate([rows, before, after, jnp.zeros((TILE - 2, width), bf16)], axis=0)

    wide = hstate.astype(f32)
    squares = jnp.sum(wide * wide, axis=1, keepdims=True)
    operand = (wide * norm_gain[1]).astype(bf16)
    product = jnp.einsum(
        "td,ykd->ytk", operand, packed[:, : 2 * LANES], preferred_element_type=f32
    )
    product = with_squares(product, squares[None], hidden).astype(bf16)
    total = swapped(product, "cb").astype(f32).sum(axis=0)
    theirs = lax.dynamic_index_in_dim(packed, lax.axis_index("cb"), 0, keepdims=False)
    theirs = theirs[:, :LANES].astype(f32)
    theirs = (
        theirs[hidden:up_at]
        + theirs[down_at - 2 * TILE : down_at - TILE]
        + theirs[down_at - TILE : down_at]
    )
    inner = activated(total, features, hidden, up_at, theirs)
    inner = sent_to_all(inner, "cb")
    down_1 = packed[:, down_at:]
    term = jnp.einsum("ytk,ykf->tf", inner[:, :, :hidden], down_1, preferred_element_type=f32)
    term = term.astype(bf16)
    share_rows = block // blocks_z
    part = swapped(term.reshape(blocks_z, share_rows, width), "ra_0").astype(f32).sum(axis=0)
    own = lax.dynamic_slice_in_dim(hstate, share_rows * at_z, share_rows, 0).astype(f32)
    fresh = (residual_scale * own + part * down_scale[1]).astype(bf16)
    fresh = sent_to_all(fresh, "ra_0").reshape(block, width)
    return sent_to_all(fresh, "ra_1").reshape(length, width)


def solution(mesh):
    split = Mesh(mesh.devices.reshape(16, 8, mesh.shape["cb"]), ("ra_0", "ra_1", "cb"))
    return jax.shard_map(
        both_layers,
        mesh=split,
        in_specs=(
            P(None, "cb"),
            P(None, "cb", RA),
            P(None, "cb", RA),
            P(None, RA, "cb"),
            P(None, RA),
            P(None, RA),
            P(None, "cb"),
            P(None, "cb"),
            P(None, None, RA),
            P(None, RA),
        ),
        out_specs=P(None, "cb"),
        check_vma=False,
    )
```

```python
import jax
import jax.numpy as jnp
from jax import lax
from jax.experimental import pallas as pl
from jax.sharding import Mesh
from jax.sharding import PartitionSpec as P


RA = ("ra_0", "ra_1")
LANES = 128
TILE = 8

norm_eps = 1e-06
residual_scale = 0.25


def swapped(pieces, axes):
    return lax.all_to_all(pieces, axes, 0, 0, tiled=True)


def sent_to_all(value, axes):
    copies = jnp.broadcast_to(value[None], (lax.axis_size(axes), *value.shape))
    return swapped(copies, axes)


def padded_to(value, size, axis):
    widths = [(0, 0)] * value.ndim
    widths[axis] = (0, size - value.shape[axis])
    return jnp.pad(value, widths)


def gathered_in_steps(own, axis):
    size = lax.axis_size(axis)

    def taken_from(value, away):
        return lax.ppermute(value, axis, [((i + away) % size, i) for i in range(size)])

    far = taken_from(own, 4)
    ahead = taken_from(own, 2)
    behind = taken_from(own, -2)
    odd_ahead = taken_from(jnp.concatenate([own, ahead]), 1)
    odd_behind = taken_from(jnp.concatenate([own, behind]), -1)
    return jnp.concatenate([own, ahead, behind, far, odd_ahead, odd_behind])


def with_neighbours(rows, blocks):
    width = rows.shape[1]
    main = rows.reshape(blocks, -1, width)
    nothing = jnp.zeros((1, width), rows.dtype)
    before = jnp.concatenate([nothing, main[:-1, -1]], axis=0)[:, None]
    after = jnp.concatenate([main[1:, 0], nothing], axis=0)[:, None]
    rest = jnp.zeros((blocks, TILE - 2, width), rows.dtype)
    return jnp.concatenate([main, before, after, rest], axis=1)


def split_in_two(value):
    high = lax.reduce_precision(value, 8, 7)
    return high, value - high


def split_in_three(value):
    first, rest = split_in_two(value)
    second, third = split_in_two(rest)
    return jnp.concatenate([first, second, third], axis=0).astype(jnp.bfloat16)


def with_squares(product, squares, hidden):
    high, low = split_in_two(squares)
    column = lax.broadcasted_iota(jnp.int32, product.shape, product.ndim - 1)
    product = jnp.where(column == hidden, high, product)
    return jnp.where(column == hidden + 1, low, product)


def first_products(tokens, gain, gate_weight, up_weight, blocks):
    length, width = tokens.shape
    hidden = gate_weight.shape[1]
    block = length // blocks

    def kernel(tokens_ref, gain_ref, gate_ref, up_ref, out_ref):
        wide = tokens_ref[...].astype(jnp.float32)
        squares = jnp.sum(wide * wide, axis=1, keepdims=True)
        operand = (wide * gain_ref[0:1]).astype(jnp.bfloat16)
        rest = jnp.zeros((LANES - hidden, width), jnp.float32)
        weight = jnp.concatenate([gate_ref[0], rest, up_ref[0], rest], axis=0).astype(jnp.bfloat16)
        product = lax.dot_general(
            operand, weight, (((1,), (1,)), ((), ())), preferred_element_type=jnp.float32
        )
        high = squares.astype(jnp.bfloat16).astype(jnp.float32)
        column = lax.broadcasted_iota(jnp.int32, product.shape, 1)
        product = jnp.where(column == hidden, high, product)
        product = jnp.where(column == hidden + 1, squares - high, product)
        row = lax.broadcasted_iota(jnp.int32, (TILE, 2 * LANES), 0)
        nothing = jnp.zeros((TILE, 2 * LANES), jnp.float32)
        for j in range(blocks):
            start = j * block
            edge = nothing
            if j > 0:
                edge = jnp.where(row == 0, product[start - 1 : start], edge)
            if j < blocks - 1:
                edge = jnp.where(row == 1, product[start + block : start + block + 1], edge)
            out_ref[j] = jnp.concatenate([product[start : start + block], edge], axis=0).astype(
                jnp.bfloat16
            )

    shape = (blocks, block + TILE, 2 * LANES)
    weight_block = pl.BlockSpec((1, hidden, width), lambda i: (0, 0, 0))
    return pl.pallas_call(
        kernel,
        grid=(1,),
        in_specs=[
            pl.BlockSpec((length, width), lambda i: (0, 0)),
            pl.BlockSpec(gain.shape, lambda i: (0, 0)),
            weight_block,
            weight_block,
        ],
        out_specs=pl.BlockSpec(shape, lambda i: (0, 0, 0)),
        out_shape=jax.ShapeDtypeStruct(shape, jnp.bfloat16),
    )(tokens, gain, gate_weight, up_weight)


def activated(total, features, hidden, up_at, params):
    rows = total.shape[0] - TILE
    square_sum = total[:, hidden : hidden + 1] + total[:, hidden + 1 : hidden + 2]
    rscale = lax.rsqrt(square_sum / features + norm_eps)
    gate = total[:, :LANES] * rscale * params[4]
    upward = total[:rows, up_at : up_at + LANES] * rscale[:rows] * params[5]
    main = gate[:rows]
    before = jnp.concatenate([gate[rows : rows + 1], main[:-1]], axis=0)
    after = jnp.concatenate([main[1:], gate[rows + 1 : rows + 2]], axis=0)
    mixed = params[0] * before + params[1] * main + params[2] * after + params[3]
    return (jax.nn.silu(mixed) * upward).astype(jnp.bfloat16)


def own_params(conv_taps, conv_bias, gate_scale, up_scale):
    stacked = jnp.concatenate([conv_taps, conv_bias[None], gate_scale[None], up_scale[None]], axis=0)
    return padded_to(stacked, LANES, 1)


def both_layers(
    tokens,
    gate_weight,
    up_weight,
    down_weight,
    gate_scale,
    up_scale,
    down_scale,
    norm_gain,
    conv_taps,
    conv_bias,
):
    blocks_c, blocks_y, blocks_z = (lax.axis_size(a) for a in ("cb", "ra_1", "ra_0"))
    at_y, at_z = lax.axis_index("ra_1"), lax.axis_index("ra_0")
    length, width = tokens.shape
    hidden = gate_weight.shape[2]
    features = width * blocks_c
    block = length // blocks_y
    f32, bf16 = jnp.float32, jnp.bfloat16

    params_1 = own_params(conv_taps[1], conv_bias[1], gate_scale[1], up_scale[1])
    carried = padded_to(split_in_three(padded_to(params_1, TILE, 0)), width, 1)
    packed = jnp.concatenate(
        [
            gate_weight[1].T.astype(bf16),
            carried,
            up_weight[1].T.astype(bf16),
            down_weight[1].astype(bf16),
        ],
        axis=0,
    )
    up_at = hidden + 3 * TILE
    down_at = up_at + hidden
    packed = gathered_in_steps(packed[None], "ra_1")

    params_0 = own_params(conv_taps[0], conv_bias[0], gate_scale[0], up_scale[0])
    product = first_products(
        tokens,
        norm_gain,
        jnp.swapaxes(gate_weight, 1, 2),
        jnp.swapaxes(up_weight, 1, 2),
        blocks_c,
    )
    total = swapped(product, "cb").astype(f32).sum(axis=0)
    inner = activated(total, features, hidden, LANES, params_0)
    inner = sent_to_all(inner, "cb").reshape(length, LANES)
    down_0 = padded_to(down_weight[0], LANES, 0).astype(bf16)
    term = jnp.dot(inner, down_0, preferred_element_type=f32).astype(bf16)

    halves = 2
    groups = blocks_z // halves
    share_rows, half = block // groups, width // halves
    term = term.reshape(blocks_y, groups, share_rows, halves, half).transpose(1, 3, 0, 2, 4)
    part = swapped(term.reshape(blocks_z, blocks_y * share_rows, half), "ra_0")
    part = part.astype(f32).sum(axis=0).astype(bf16)
    part = swapped(with_neighbours(part, blocks_y), "ra_1").astype(f32).sum(axis=0)
    group, column = at_z // halves, (at_z % halves) * half

    def residual_rows(block_at, row, count):
        start = jnp.clip(block_at, 0, blocks_y - 1) * block + group * share_rows + row
        rows = lax.dynamic_slice(tokens, (start, column), (count, half))
        inside = (block_at >= 0) & (block_at < blocks_y)
        return jnp.where(inside, rows, jnp.zeros_like(rows))

    own = jnp.concatenate(
        [
            residual_rows(at_y, 0, share_rows),
            residual_rows(at_y - 1, share_rows - 1, 1),
            residual_rows(at_y + 1, 0, 1),
            jnp.zeros((TILE - 2, half), bf16),
        ],
        axis=0,
    )
    scale = lax.dynamic_slice_in_dim(down_scale[0], column, half, 0)
    fresh = (residual_scale * own.astype(f32) + part * scale).astype(bf16)
    fresh = sent_to_all(fresh, "ra_0").reshape(groups, halves, share_rows + TILE, half)
    rows = fresh[:, :, :share_rows].transpose(0, 2, 1, 3).reshape(block, width)
    before = fresh[groups - 1, :, share_rows].reshape(1, width)
    after = fresh[0, :, share_rows + 1].reshape(1, width)
    hstate = jnp.concatenate([rows, before, after, jnp.zeros((TILE - 2, width), bf16)], axis=0)

    wide = hstate.astype(f32)
    squares = jnp.sum(wide * wide, axis=1, keepdims=True)
    operand = (wide * norm_gain[1]).astype(bf16)
    product = jnp.einsum(
        "td,ykd->ytk", operand, packed[:, : 2 * LANES], preferred_element_type=f32
    )
    product = with_squares(product, squares[None], hidden).astype(bf16)
    total = swapped(product, "cb").astype(f32).sum(axis=0)
    theirs = lax.dynamic_index_in_dim(packed, lax.axis_index("cb"), 0, keepdims=False)
    theirs = theirs[hidden:up_at, :LANES].astype(f32).reshape(3, TILE, LANES)
    theirs = theirs[0] + theirs[1] + theirs[2]
    inner = activated(total, features, hidden, up_at, theirs)
    inner = sent_to_all(inner, "cb")
    down_1 = packed[:, down_at:]
    term = jnp.einsum("ytk,ykf->tf", inner[:, :, :hidden], down_1, preferred_element_type=f32)
    term = term.astype(bf16)
    share_rows = block // blocks_z
    part = swapped(term.reshape(blocks_z, share_rows, width), "ra_0").astype(f32).sum(axis=0)
    own = lax.dynamic_slice_in_dim(hstate, share_rows * at_z, share_rows, 0).astype(f32)
    fresh = (residual_scale * own + part * down_scale[1]).astype(bf16)
    fresh = sent_to_all(fresh, "ra_0").reshape(block, width)
    return sent_to_all(fresh, "ra_1").reshape(length, width)


def solution(mesh):
    split = Mesh(mesh.devices.reshape(16, 8, mesh.shape["cb"]), ("ra_0", "ra_1", "cb"))
    return jax.shard_map(
        both_layers,
        mesh=split,
        in_specs=(
            P(None, "cb"),
            P(None, "cb", RA),
            P(None, "cb", RA),
            P(None, RA, "cb"),
            P(None, RA),
            P(None, RA),
            P(None, "cb"),
            P(None, "cb"),
            P(None, None, RA),
            P(None, RA),
        ),
        out_specs=P(None, "cb"),
        check_vma=False,
    )
```
